32 devices in a mesh: sp: 16 (over z, y, x), tp: 2 (over core).
Axes of the slice: x: 2, y: 2, z: 4, core: 2. Of those that a mesh axis runs over, the one named last changes fastest.
Arguments:
- stream: bfloat16 [4096, 2048], P('sp', 'tp'), may hold values from -6 to 6
- out_grad: bfloat16 [4096, 2048], P('sp', 'tp'), may hold values from -6 to 6
- gate_in: bfloat16 [4096, 1024], P('sp', 'tp'), may hold values from -6 to 6
- conv_gate: bfloat16 [4096, 1024], P('sp', 'tp'), may hold values from -6 to 6
- conv_value: bfloat16 [4096, 1024], P('sp', 'tp'), may hold values from -6 to 6
- taps: float32 [3, 1024], P(None, 'tp'), may hold values from -3.5 to 3.5
- w_out: bfloat16 [2048, 1024], P(None, 'tp'), may hold values from -0.1875 to 0.1875
- route_ids: int32 [4096, 2], P('sp'), may hold values from 0 to 15, all different within a row; in each aligned block of 256 rows (0 to 255, 256 to 511, ...) at most 64 rows name the same one
- route_weights: float32 [4096, 2], P('sp'), may hold values from 0.1 to 1
- w_gate: bfloat16 [16, 2048, 1024], P('sp', None, 'tp'), may hold values from -0.125 to 0.125
- w_up: bfloat16 [16, 2048, 1024], P('sp', None, 'tp'), may hold values from -0.125 to 0.125
- w_down: bfloat16 [16, 1024, 2048], P('sp', 'tp'), may hold values from -0.1875 to 0.1875
Outputs:
- stream_grad: bfloat16 [4096, 2048], P('sp', 'tp')
- gate_in_grad: bfloat16 [4096, 1024], P('sp', 'tp')
- conv_gate_grad: bfloat16 [4096, 1024], P('sp', 'tp')
- conv_value_grad: bfloat16 [4096, 1024], P('sp', 'tp')
- w_out_grad: float32 [2048, 1024], P('sp', 'tp')
- w_gate_grad: float32 [16, 2048, 1024], P('sp', None, 'tp')
- w_up_grad: float32 [16, 2048, 1024], P('sp', None, 'tp')
- w_down_grad: float32 [16, 1024, 2048], P('sp', 'tp')
The draws below stay inside these ranges and needn't reach their ends.
Inputs may be any that keep to these rules, and one draw needn't show every extreme that they name: `route_ids`: the ids of one token differ. Within each aligned block of 256 tokens (the rows of one index of sp), no expert is named by more than 64 routes, and in every draw some expert is named by exactly 64 routes of some block.
All inputs are finite; a program needn't handle non-finite values.
Results may differ from the reference program's by a relative error of at most 0.009.
Values may be sent and summed in bfloat16 or wider, within the bound.
A program may use at most 128 MiB of HBM per device.

```python
import math
import jax
import jax.numpy as jnp
import numpy as np
from jax import lax

D = 2048
CW = 1024
FF = 1024
TOP = 2
TAPS = 3
EXPERTS = 16
TOK_DEV = 256
TOKENS = 4096
CAP = 64
EXPERT_ROWS = 1024
N_SP = 16
N_TP = 2


def strengthened(drawn, rng, source, target, parts, factor):
    owner, partner = [(jnp.arange(drawn.shape[position]) // (drawn.shape[position] // parts)).reshape([-1 if axis == position else 1 for axis in range(drawn.ndim)]) for position in (source, target)]
    chosen = jax.random.permutation(rng, parts)[partner]
    strong = (owner == chosen) | (owner == (partner + parts // 2) % parts)
    return jnp.where(strong, factor * drawn, drawn)


def level_of(own_key, dims, pieces, smallest, high):
    def one(position, blocks):
        steps = jax.random.uniform(jax.random.fold_in(jax.random.fold_in(own_key, 6), position), (blocks,), jnp.float32, smallest / len(pieces), high / len(pieces))
        return jnp.repeat(jnp.exp(steps), dims[position] // blocks).reshape((-1,) + (1,) * (len(dims) - position - 1))

    factor_of = one(*pieces[0])
    for cut in pieces[1:]:
        factor_of = factor_of * one(*cut)
    return factor_of


def deal_out(stream_key, own, number, rows, count, top, bound, lean):
    ranking = jax.random.permutation(stream_key, count)
    packed, usual = shares(count, rows * top, bound, lean, True), shares(count, rows * top, bound, lean, False)
    places = jnp.arange(count)

    def named(sizes, turn):
        used = int((sizes > 0).sum())
        fixed = max(1, used // 4)
        passed = fixed + (places - fixed + turn * (used - fixed)) % max(1, count - fixed)
        return jnp.zeros((count,), jnp.int32).at[ranking[jnp.where(places < fixed, places, passed)]].set(jnp.asarray(sizes, jnp.int32))

    sizes = jnp.where(number % 4 == 0, named(packed, number // 4), named(usual, number - number // 4 - 1))
    mixed = jax.random.permutation(jax.random.fold_in(own, 3), count)
    giver, taker = mixed[0:count // 2 * 2:2], mixed[1:count // 2 * 2:2]
    room = jnp.minimum(sizes[giver] - 1, bound - sizes[taker]) // 2
    room = jnp.where((giver == ranking[0]) | (taker == ranking[0]) | (sizes[taker] == 0), 0, jnp.maximum(room, 0))
    passed = jax.random.randint(jax.random.fold_in(own, 4), (count // 2,), 0, 1 << 20) % (room + 1)
    sizes = sizes.at[giver].add(-passed).at[taker].add(passed)
    items = jnp.searchsorted(jnp.cumsum(sizes), jnp.arange(rows * top), side="right").astype(jnp.int32)
    listing = items.reshape(top, rows).T
    listing = listing[jax.random.permutation(jax.random.fold_in(own, 1), rows)]
    turn = jax.random.randint(jax.random.fold_in(own, 2), (rows, 1), 0, top)
    return jnp.take_along_axis(listing, (jnp.arange(top)[None, :] + turn) % top, axis=1)


def shares(amount, total, most, skew, full):
    loads = [(1 << 20) // math.isqrt(grade ** skew) + 1 for grade in range(1, amount + 1)]
    largest = most if full else min(most, max(-(-total // amount), total * loads[0] // sum(loads)))
    least = 1 if total - largest >= amount - 1 else 0
    given, rest = [largest] + [least] * (amount - 1), total - largest - least * (amount - 1)
    while rest > 0:
        free = [i for i in range(1, amount) if given[i] < largest] or [i for i in range(1, amount) if given[i] < most]
        whole, left = sum([loads[i] for i in free]), rest
        for i in free:
            addition = min(most - given[i], max(1, left * loads[i] // whole), rest)
            given[i] = given[i] + addition
            rest = rest - addition
    return np.array(given)


def scatter_about(own_key, dims, scale, limit, split=(), kind=jnp.bfloat16):
    array = scale * jax.random.normal(own_key, dims, jnp.float32)
    if split:
        array = array * level_of(own_key, dims, split, -0.22, 0.18)
    return jnp.clip(array, -limit, limit).astype(kind)


def gaussian_with(rng, extent, width, most, pieces, heavy, held_as=jnp.bfloat16):
    result = width * jax.random.normal(rng, extent, jnp.float32)
    if pieces:
        result = result * level_of(rng, extent, pieces, -0.22, 0.18)
    return jnp.clip(strengthened(result, jax.random.fold_in(rng, 3), *heavy), -most, most).astype(held_as)


def setup_inputs(seed: int = 0) -> dict:
    key_list = jax.random.split(jax.random.key(seed), 13)
    stream = scatter_about(key_list[0], (TOKENS, D), 1.0, 6.0, ((0, 16), (1, 2)))
    out_grad = gaussian_with(key_list[1], (TOKENS, D), 1.0, 6.0, ((0, 16), (1, 2)), (0, 1, 16, 2.0))
    gate_in = scatter_about(key_list[2], (TOKENS, CW), 1.0, 6.0, ((0, 16), (1, 2)))
    conv_gate = scatter_about(key_list[3], (TOKENS, CW), 1.0, 6.0, ((0, 16), (1, 2)))
    conv_value = scatter_about(key_list[4], (TOKENS, CW), 1.0, 6.0, ((0, 16), (1, 2)))
    taps = scatter_about(key_list[5], (TAPS, CW), TAPS ** -0.5, 3.5, ((1, 2),), jnp.float32)
    w_out = scatter_about(key_list[6], (D, CW), CW ** -0.5, 0.1875, ((1, 2),))
    route_ids_keys = jax.random.split(jax.random.fold_in(key_list[7], 1), TOKENS // TOK_DEV)
    route_ids_turns = jax.random.permutation(jax.random.fold_in(key_list[7], 3), TOKENS // TOK_DEV)
    route_ids = jax.vmap(lambda own, number: deal_out(jax.random.fold_in(key_list[7], 2), own, number, TOK_DEV, EXPERTS, TOP, CAP, 2))(route_ids_keys, route_ids_turns).reshape((TOKENS, TOP))
    route_weights = jnp.clip(0.1 + 0.9 * jax.random.uniform(key_list[8], (TOKENS, TOP), jnp.float32) ** level_of(key_list[8], (TOKENS, TOP), ((0, 16),), -0.2, 0.2), 0.1, 1.0)
    w_gate = scatter_about(key_list[9], (EXPERTS, D, FF), D ** -0.5, 0.125, ((0, 16), (2, 2)))
    w_up = scatter_about(key_list[10], (EXPERTS, D, FF), D ** -0.5, 0.125, ((0, 16), (2, 2)))
    w_down = scatter_about(key_list[11], (EXPERTS, FF, D), FF ** -0.5, 0.1875, ((0, 16), (1, 2)))
    return {"stream": stream, "out_grad": out_grad, "gate_in": gate_in, "conv_gate": conv_gate, "conv_value": conv_value, "taps": taps, "w_out": w_out, "route_ids": route_ids, "route_weights": route_weights, "w_gate": w_gate, "w_up": w_up, "w_down": w_down}


def expert_step(carry_rows, stream_pad, cot_pad):
    table_row, gate_weight, up_weight, down_weight = carry_rows
    routes_total = TOKENS * TOP
    token_index = jnp.where(table_row < routes_total, table_row // TOP, TOKENS).astype(jnp.int32)
    expert_in = stream_pad[token_index]
    expert_cot = cot_pad[table_row]
    pre_gate = jnp.dot(expert_in, gate_weight, preferred_element_type=jnp.float32)
    pre_up = jnp.dot(expert_in, up_weight, preferred_element_type=jnp.float32)
    sigmoid_gate = jax.nn.sigmoid(pre_gate)
    silu_gate = pre_gate * sigmoid_gate
    hidden = (silu_gate * pre_up).astype(jnp.bfloat16)
    hidden_grad = jnp.dot(expert_cot, down_weight.T, preferred_element_type=jnp.float32)
    down_grad = jnp.dot(hidden.T, expert_cot, preferred_element_type=jnp.float32)
    up_grad = (hidden_grad * silu_gate).astype(jnp.bfloat16)
    gate_grad = (hidden_grad * pre_up * sigmoid_gate * (1.0 + pre_gate * (1.0 - sigmoid_gate))).astype(jnp.bfloat16)
    gate_w_grad = jnp.dot(expert_in.T, gate_grad, preferred_element_type=jnp.float32)
    up_w_grad = jnp.dot(expert_in.T, up_grad, preferred_element_type=jnp.float32)
    block_width = FF // N_TP
    running = jnp.zeros((EXPERT_ROWS, D), jnp.float32)
    for block_index in range(N_TP):
        lower = block_index * block_width
        upper = lower + block_width
        partial_term = jnp.dot(gate_grad[:, lower:upper], gate_weight[:, lower:upper].T, preferred_element_type=jnp.float32)
        partial_term = partial_term + jnp.dot(up_grad[:, lower:upper], up_weight[:, lower:upper].T, preferred_element_type=jnp.float32)
        rounded = lax.optimization_barrier(partial_term.astype(jnp.bfloat16))
        running = running + rounded.astype(jnp.float32)
    return gate_w_grad, up_w_grad, down_grad, running.astype(jnp.bfloat16)


def reference(stream, out_grad, gate_in, conv_gate, conv_value, taps, w_out, route_ids, route_weights, w_gate, w_up, w_down):
    prod_rows = conv_gate.astype(jnp.float32) * conv_value.astype(jnp.float32)
    padded = jnp.concatenate([jnp.zeros((TAPS - 1, CW), jnp.float32), prod_rows], axis=0)
    conv_sum = jnp.zeros((TOKENS, CW), jnp.float32)
    for tap_index in range(TAPS):
        conv_sum = conv_sum + taps[tap_index][None, :] * padded[tap_index:tap_index + TOKENS]
    mixer_out = (gate_in.astype(jnp.float32) * conv_sum).astype(jnp.bfloat16)

    routes_dev = TOK_DEV * TOP
    route_block = route_ids.reshape(N_SP, routes_dev)
    one_hot = (route_block[:, :, None] == jnp.arange(EXPERTS, dtype=jnp.int32)[None, None, :]).astype(jnp.int32)
    slot_pos = jnp.sum(jnp.cumsum(one_hot, axis=1) * one_hot, axis=2) - 1
    source_index = jnp.arange(N_SP, dtype=jnp.int32)[:, None]
    flat_slot = (route_block * EXPERT_ROWS + source_index * CAP + slot_pos).reshape(-1).astype(jnp.int32)
    routes_total = TOKENS * TOP
    table = jnp.full((EXPERTS * EXPERT_ROWS,), routes_total, jnp.int32)
    table = table.at[flat_slot].set(jnp.arange(routes_total, dtype=jnp.int32))
    table = table.reshape(EXPERTS, EXPERT_ROWS)

    stream_pad = jnp.concatenate([stream, jnp.zeros((1, D), jnp.bfloat16)], axis=0)
    scaled = (route_weights[:, :, None] * out_grad[:, None, :].astype(jnp.float32)).astype(jnp.bfloat16)
    cot_pad = jnp.concatenate([scaled.reshape(routes_total, D), jnp.zeros((1, D), jnp.bfloat16)], axis=0)

    def per_expert(carry_rows):
        return expert_step(carry_rows, stream_pad, cot_pad)

    w_gate_grad, w_up_grad, w_down_grad, row_grad = lax.map(per_expert, (table, w_gate, w_up, w_down))
    row_flat = row_grad.reshape(EXPERTS * EXPERT_ROWS, D)
    route_rows = row_flat[flat_slot].astype(jnp.float32).reshape(TOKENS, TOP, D)
    input_grad = jnp.sum(route_rows, axis=1)
    stream_grad = (out_grad.astype(jnp.float32) + input_grad).astype(jnp.bfloat16)

    w_out_grad = jnp.dot(stream_grad.T, mixer_out, preferred_element_type=jnp.float32)
    mixer_grad = jnp.dot(stream_grad, w_out, preferred_element_type=jnp.float32).astype(jnp.bfloat16)
    gate_in_grad = (mixer_grad.astype(jnp.float32) * conv_sum).astype(jnp.bfloat16)
    conv_inner = mixer_grad.astype(jnp.float32) * gate_in.astype(jnp.float32)
    padded_back = jnp.concatenate([conv_inner, jnp.zeros((TAPS - 1, CW), jnp.float32)], axis=0)
    prod_grad = jnp.zeros((TOKENS, CW), jnp.float32)
    for tap_index in range(TAPS):
        offset = TAPS - 1 - tap_index
        prod_grad = prod_grad + taps[tap_index][None, :] * padded_back[offset:offset + TOKENS]
    conv_gate_grad = (prod_grad * conv_value.astype(jnp.float32)).astype(jnp.bfloat16)
    conv_value_grad = (prod_grad * conv_gate.astype(jnp.float32)).astype(jnp.bfloat16)
    return (stream_grad, gate_in_grad, conv_gate_grad, conv_value_grad, w_out_grad, w_gate_grad, w_up_grad, w_down_grad)
```

```python
import functools

import jax
import jax.numpy as jnp
from jax import lax
from jax.experimental import pallas as pl
from jax.experimental.pallas import tpu as pltpu
from jax.sharding import PartitionSpec as P

MESH = pl.DeviceIdType.MESH
GROUPS = 4
F32 = jnp.float32
BF16 = jnp.bfloat16


def passed_along(shard, axis, by):
    count = lax.axis_size(axis)
    pairs = [(i, i + by) for i in range(count) if 0 <= i + by < count]
    return lax.ppermute(shard, axis, pairs)


def dot(a, b, ca, cb):
    return lax.dot_general(a, b, (((ca,), (cb,)), ((), ())), preferred_element_type=F32)


def expert_kernel(
    count,
    cap,
    send_rows,
    send_cot,
    wg_hbm,
    wu_hbm,
    wd_hbm,
    back_out,
    gate_out,
    up_out,
    down_out,
    rows,
    cot,
    wg,
    wu,
    wd,
    pre_g,
    pre_u,
    hidden,
    gg,
    ug,
    part_out,
    part_in,
    ret,
    back,
    gate_f,
    up_f,
    down_f,
    w_sem,
    out_sem,
    send_sem,
    recv_sem,
    fsend_sem,
    frecv_sem,
    psend_sem,
    precv_sem,
    rsend_sem,
    rrecv_sem,
):
    me = lax.axis_index("sp")
    half = lax.axis_index("tp")
    other = 1 - half
    per = count // GROUPS
    height = per * cap
    width = rows.shape[2]
    tall = cap * count

    loads = []
    for n, (a, b) in enumerate(((wg_hbm, wg), (wu_hbm, wu), (wd_hbm, wd))):
        load = pltpu.make_async_copy(a.at[0], b, w_sem.at[n])
        load.start()
        loads.append(load)

    barrier = pltpu.get_barrier_semaphore()

    @pl.loop(1, count)
    def _(k):
        pl.semaphore_signal(
            barrier, inc=1, device_id=(lax.rem(me + k, count), half), device_id_type=MESH
        )

    pl.semaphore_signal(barrier, inc=1, device_id=(me, other), device_id_type=MESH)
    pl.semaphore_wait(barrier, count)

    def block(k):
        return pl.ds(pl.multiple_of(k * cap, cap), cap)

    def out_copy(which, src, dst, k):
        return pltpu.make_async_remote_copy(
            src_ref=src.at[block(k)],
            dst_ref=dst.at[half, block(k)],
            send_sem=send_sem.at[which, k],
            recv_sem=recv_sem.at[which, k],
            device_id=(lax.rem(me + k, count), half),
            device_id_type=MESH,
        )

    def pass_copy(which, src, k):
        return pltpu.make_async_remote_copy(
            src_ref=src,
            dst_ref=(rows if which == 0 else cot).at[half, block(k)],
            send_sem=fsend_sem.at[which, k],
            recv_sem=frecv_sem.at[which, k],
            device_id=(me, other),
            device_id_type=MESH,
        )

    def back_copy(k):
        return pltpu.make_async_remote_copy(
            src_ref=ret.at[block(k)],
            dst_ref=back.at[block(k)],
            send_sem=rsend_sem.at[k],
            recv_sem=rrecv_sem.at[k],
            device_id=(lax.rem(me - k + count, count), half),
            device_id_type=MESH,
        )

    def part_copy(g):
        at = pl.ds(pl.multiple_of(g * height, height), height)
        return pltpu.make_async_remote_copy(
            src_ref=part_out.at[at],
            dst_ref=part_in.at[at],
            send_sem=psend_sem.at[g],
            recv_sem=precv_sem.at[g],
            device_id=(me, other),
            device_id_type=MESH,
        )

    pairs = ((send_rows, rows), (send_cot, cot))
    for which, (src, dst) in enumerate(pairs):
        pass_copy(which, src.at[block(0)], 0).start()

        @pl.loop(1, count)
        def _(k):
            out_copy(which, src, dst, k).start()

    for which, (src, dst) in enumerate(pairs):
        dst[half, pl.ds(0, cap)] = src[pl.ds(0, cap)]
    for load in loads:
        load.wait()

    def gather_group(which, g):
        src, dst = pairs[which]

        @pl.loop(0, per)
        def _(j):
            k = g * per + j

            @pl.when(k > 0)
            def _():
                out_copy(which, src, dst, k).wait_recv()
                pass_copy(which, dst.at[half, block(k)], k).start()

        @pl.loop(0, per)
        def _(j):
            k = g * per + j
            pass_copy(which, dst.at[half, block(k)], k).wait_recv()

    @pl.loop(0, GROUPS)
    def _(g):
        gather_group(0, g)
        at = pl.ds(pl.multiple_of(g * height, height), height)
        left, right = rows[0, at], rows[1, at]
        pre_g[at] = dot(left, wg[:width], 1, 0) + dot(right, wg[width:], 1, 0)
        pre_u[at] = dot(left, wu[:width], 1, 0) + dot(right, wu[width:], 1, 0)

    mine_at = pl.ds(pl.multiple_of(half * width, width), width)
    other_at = pl.ds(pl.multiple_of(other * width, width), width)

    @pl.loop(0, GROUPS)
    def _(g):
        gather_group(1, g)
        at = pl.ds(pl.multiple_of(g * height, height), height)
        grad = dot(cot[0, at], wd[:, :width], 1, 1) + dot(cot[1, at], wd[:, width:], 1, 1)
        pg, pu = pre_g[at], pre_u[at]
        sig = jax.nn.sigmoid(pg)
        silu = pg * sig
        hidden[at] = (silu * pu).astype(BF16)
        ug_now = (grad * silu).astype(BF16)
        gg_now = (grad * pu * sig * (1.0 + pg * (1.0 - sig))).astype(BF16)
        ug[at] = ug_now
        gg[at] = gg_now
        far = dot(gg_now, wg[other_at], 1, 1) + dot(ug_now, wu[other_at], 1, 1)
        part_out[at] = far.astype(BF16)
        part_copy(g).start()
        near = dot(gg_now, wg[mine_at], 1, 1) + dot(ug_now, wu[mine_at], 1, 1)
        near = near.astype(BF16).astype(F32)
        part_copy(g).wait_recv()
        ret[at] = (near + part_in[at].astype(F32)).astype(BF16)

        @pl.loop(0, per)
        def _(j):
            k = g * per + j

            @pl.when(k > 0)
            def _():
                back_copy(k).start()

    back[pl.ds(0, cap)] = ret[pl.ds(0, cap)]

    tile = 256
    per_half = width // tile

    @pl.loop(0, 2 * per_half)
    def _(t):
        h, c = t // per_half, lax.rem(t, per_half)
        cols = pl.ds(pl.multiple_of(c * tile, tile), tile)
        to = pl.ds(pl.multiple_of(t * tile, tile), tile)
        x = rows[h, :, cols].T
        gate_f[to] = dot(x, gg[...], 1, 0)
        up_f[to] = dot(x, ug[...], 1, 0)

    stores = [
        pltpu.make_async_copy(gate_f, gate_out.at[0], out_sem.at[0]),
        pltpu.make_async_copy(up_f, up_out.at[0], out_sem.at[1]),
    ]
    for store in stores:
        store.start()

    hid_tile = min(256, hidden.shape[1])

    @pl.loop(0, hidden.shape[1] // hid_tile)
    def _(t):
        to = pl.ds(pl.multiple_of(t * hid_tile, hid_tile), hid_tile)
        x = hidden[:, to].T
        for h in range(2):
            down_f[to, h * width : (h + 1) * width] = dot(x, cot[h], 1, 0)

    stores.append(pltpu.make_async_copy(down_f, down_out.at[0], out_sem.at[2]))
    stores[-1].start()

    for which, (src, dst) in enumerate(pairs):

        @pl.loop(0, count)
        def _(k):
            @pl.when(k > 0)
            def _():
                out_copy(which, src, dst, k).wait_send()

            pass_copy(which, dst.at[half, block(k)], k).wait_send()

    @pl.loop(0, GROUPS)
    def _(g):
        part_copy(g).wait_send()

    @pl.loop(1, count)
    def _(k):
        back_copy(k).wait_send()
        back_copy(k).wait_recv()

    back_out[...] = back[...]
    for store in stores:
        store.wait()


def expert_pass(send_rows, send_cot, w_gate, w_up, w_down, cap):
    tall, width = send_rows.shape
    count = lax.axis_size("sp")
    deep, hid = w_gate.shape[1:]
    vmem = pl.BlockSpec(memory_space=pltpu.VMEM)
    anywhere = pl.BlockSpec(memory_space=pl.ANY)
    dma = pltpu.SemaphoreType.DMA
    return pl.pallas_call(
        functools.partial(expert_kernel, count, cap),
        out_shape=(
            jax.ShapeDtypeStruct((tall, width), BF16),
            jax.ShapeDtypeStruct((1, deep, hid), F32),
            jax.ShapeDtypeStruct((1, deep, hid), F32),
            jax.ShapeDtypeStruct((1, hid, deep), F32),
        ),
        in_specs=[vmem, vmem, anywhere, anywhere, anywhere],
        out_specs=(vmem, anywhere, anywhere, anywhere),
        scratch_shapes=[
            pltpu.VMEM((2, tall, width), BF16),
            pltpu.VMEM((2, tall, width), BF16),
            pltpu.VMEM((deep, hid), BF16),
            pltpu.VMEM((deep, hid), BF16),
            pltpu.VMEM((hid, deep), BF16),
            pltpu.VMEM((tall, hid), F32),
            pltpu.VMEM((tall, hid), F32),
            pltpu.VMEM((tall, hid), BF16),
            pltpu.VMEM((tall, hid), BF16),
            pltpu.VMEM((tall, hid), BF16),
            pltpu.VMEM((tall, width), BF16),
            pltpu.VMEM((tall, width), BF16),
            pltpu.VMEM((tall, width), BF16),
            pltpu.VMEM((tall, width), BF16),
            pltpu.VMEM((deep, hid), F32),
            pltpu.VMEM((deep, hid), F32),
            pltpu.VMEM((hid, deep), F32),
            dma((3,)),
            dma((3,)),
            dma((2, count)),
            dma((2, count)),
            dma((2, count)),
            dma((2, count)),
            dma((GROUPS,)),
            dma((GROUPS,)),
            dma((count,)),
            dma((count,)),
        ],
        compiler_params=pltpu.CompilerParams(
            collective_id=0, has_side_effects=True, vmem_limit_bytes=60 * 1024 * 1024
        ),
    )(send_rows, send_cot, w_gate, w_up, w_down)


def shards(
    stream,
    out_grad,
    gate_in,
    conv_gate,
    conv_value,
    taps,
    w_out,
    route_ids,
    route_weights,
    w_gate,
    w_up,
    w_down,
):
    tok_rows, half_width = stream.shape
    top_count = route_ids.shape[1]
    experts = w_gate.shape[0] * lax.axis_size("sp")
    capacity = 4 * tok_rows // experts
    route_total = tok_rows * top_count
    slots = experts * capacity
    me = lax.axis_index("sp")
    relative = lax.rem(route_ids - me + experts, experts)
    flat = relative.reshape(route_total)
    one_hot = flat[:, None] == jnp.arange(experts, dtype=jnp.int32)[None, :]
    order = jnp.arange(route_total, dtype=jnp.int32)
    earlier = (order[:, None] > order[None, :]).astype(BF16)
    ranks = dot(earlier, one_hot.astype(BF16), 1, 0)
    slot_pos = jnp.sum(jnp.where(one_hot, ranks, 0.0), axis=1).astype(jnp.int32)
    slot_of = (flat * capacity + slot_pos).reshape(tok_rows, top_count)
    places = jnp.arange(slots, dtype=jnp.int32)
    hits = [slot_of[:, k][None, :] == places[:, None] for k in range(top_count)]
    slot_weight = sum(
        jnp.sum(jnp.where(hits[k], route_weights[:, k][None, :], 0.0), axis=1)
        for k in range(top_count)
    )
    pick = functools.reduce(jnp.logical_or, hits).astype(BF16)
    send_rows = dot(pick, stream, 1, 0).astype(BF16)
    send_cot = (slot_weight[:, None] * dot(pick, out_grad, 1, 0)).astype(BF16)
    back, gate_w_grad, up_w_grad, down_w_grad = expert_pass(
        send_rows, send_cot, w_gate, w_up, w_down, capacity
    )
    input_grad = dot(pick, back, 0, 0)
    stream_half = (out_grad.astype(jnp.float32) + input_grad).astype(jnp.bfloat16)
    stream_whole = lax.all_gather(stream_half, "tp", axis=1, tiled=True)
    mixer_grad = jnp.dot(stream_whole, w_out, preferred_element_type=jnp.float32).astype(
        jnp.bfloat16
    )
    depth = taps.shape[0]
    channels = conv_gate.shape[1]
    prod_rows = conv_gate.astype(jnp.float32) * conv_value.astype(jnp.float32)
    left_rows = passed_along(prod_rows[tok_rows - depth + 1 :], "sp", 1)
    padded = jnp.concatenate([left_rows, prod_rows], axis=0)
    conv_sum = jnp.zeros((tok_rows, channels), jnp.float32)
    for tap_index in range(depth):
        conv_sum = conv_sum + taps[tap_index][None, :] * padded[tap_index : tap_index + tok_rows]
    mixer_out = (gate_in.astype(jnp.float32) * conv_sum).astype(jnp.bfloat16)
    out_proj_grad = lax.psum_scatter(
        dot(stream_whole, mixer_out, 0, 0).astype(BF16),
        "sp",
        scatter_dimension=0,
        tiled=True,
    ).astype(F32)
    mixer_wide = mixer_grad.astype(jnp.float32)
    gate_in_grad = (mixer_wide * conv_sum).astype(jnp.bfloat16)
    conv_inner = mixer_wide * gate_in.astype(jnp.float32)
    right_rows = passed_along(conv_inner[: depth - 1], "sp", -1)
    padded_back = jnp.concatenate([conv_inner, right_rows], axis=0)
    prod_grad = jnp.zeros((tok_rows, channels), jnp.float32)
    for tap_index in range(depth):
        offset = depth - 1 - tap_index
        prod_grad = prod_grad + taps[tap_index][None, :] * padded_back[offset : offset + tok_rows]
    conv_gate_grad = (prod_grad * conv_value.astype(jnp.float32)).astype(jnp.bfloat16)
    conv_value_grad = (prod_grad * conv_gate.astype(jnp.float32)).astype(jnp.bfloat16)
    return (
        stream_half,
        gate_in_grad,
        conv_gate_grad,
        conv_value_grad,
        out_proj_grad,
        gate_w_grad,
        up_w_grad,
        down_w_grad,
    )


def solution(mesh):
    placed = (
        P("sp", "tp"),
        P("sp", "tp"),
        P("sp", "tp"),
        P("sp", "tp"),
        P("sp", "tp"),
        P(None, "tp"),
        P(None, "tp"),
        P("sp", None),
        P("sp", None),
        P("sp", None, "tp"),
        P("sp", None, "tp"),
        P("sp", "tp", None),
    )
    return jax.shard_map(
        shards,
        mesh=mesh,
        in_specs=placed,
        out_specs=(
            P("sp", "tp"),
            P("sp", "tp"),
            P("sp", "tp"),
            P("sp", "tp"),
            P("sp", "tp"),
            P("sp", None, "tp"),
            P("sp", None, "tp"),
            P("sp", "tp", None),
        ),
        check_vma=False,
    )
```

```python
import functools

import jax
import jax.numpy as jnp
from jax import lax
from jax.experimental import pallas as pl
from jax.experimental.pallas import tpu as pltpu
from jax.sharding import PartitionSpec as P

MESH = pl.DeviceIdType.MESH
GROUPS = 4
F32 = jnp.float32
BF16 = jnp.bfloat16


def passed_along(shard, axis, by):
    count = lax.axis_size(axis)
    pairs = [(i, i + by) for i in range(count) if 0 <= i + by < count]
    return lax.ppermute(shard, axis, pairs)


def dot(a, b, ca, cb):
    return lax.dot_general(a, b, (((ca,), (cb,)), ((), ())), preferred_element_type=F32)


def team_size(count):
    size = 1
    while size * size < count:
        size *= 2
    return size


def expert_kernel(
    count,
    cap,
    send_rows,
    send_cot,
    wg_hbm,
    wu_hbm,
    wd_hbm,
    mix_in,
    back_out,
    mix_out,
    gate_out,
    up_out,
    down_out,
    rows,
    cot,
    wg,
    wu,
    wd,
    pre_g,
    pre_u,
    hidden,
    gg,
    ug,
    part_out,
    part_in,
    ret,
    back,
    gate_f,
    up_f,
    down_f,
    mix,
    w_sem,
    out_sem,
    send_sem,
    recv_sem,
    fsend_sem,
    frecv_sem,
    psend_sem,
    precv_sem,
    rsend_sem,
    rrecv_sem,
    msend_sem,
    mrecv_sem,
):
    me = lax.axis_index("sp")
    half = lax.axis_index("tp")
    other = 1 - half
    per = count // GROUPS
    height = per * cap
    width = rows.shape[2]
    tall = cap * count

    loads = []
    for n, (a, b) in enumerate(((wg_hbm, wg), (wu_hbm, wu), (wd_hbm, wd))):
        load = pltpu.make_async_copy(a.at[0], b, w_sem.at[n])
        load.start()
        loads.append(load)

    barrier = pltpu.get_barrier_semaphore()

    @pl.loop(1, count)
    def _(k):
        pl.semaphore_signal(
            barrier, inc=1, device_id=(lax.rem(me + k, count), half), device_id_type=MESH
        )

    pl.semaphore_signal(barrier, inc=1, device_id=(me, other), device_id_type=MESH)
    pl.semaphore_wait(barrier, count)

    def block(k):
        return pl.ds(pl.multiple_of(k * cap, cap), cap)

    def out_copy(which, src, dst, k):
        return pltpu.make_async_remote_copy(
            src_ref=src.at[block(k)],
            dst_ref=dst.at[half, block(k)],
            send_sem=send_sem.at[which, k],
            recv_sem=recv_sem.at[which, k],
            device_id=(lax.rem(me + k, count), half),
            device_id_type=MESH,
        )

    def pass_copy(which, src, k):
        return pltpu.make_async_remote_copy(
            src_ref=src,
            dst_ref=(rows if which == 0 else cot).at[half, block(k)],
            send_sem=fsend_sem.at[which, k],
            recv_sem=frecv_sem.at[which, k],
            device_id=(me, other),
            device_id_type=MESH,
        )

    def back_copy(k):
        return pltpu.make_async_remote_copy(
            src_ref=ret.at[block(k)],
            dst_ref=back.at[block(k)],
            send_sem=rsend_sem.at[k],
            recv_sem=rrecv_sem.at[k],
            device_id=(lax.rem(me - k + count, count), half),
            device_id_type=MESH,
        )

    team = team_size(count)
    place = lax.rem(me, team)
    toks = mix_in.shape[0]

    def mix_copy(j):
        return pltpu.make_async_remote_copy(
            src_ref=mix_in,
            dst_ref=mix.at[pl.ds(pl.multiple_of(j * toks, toks), toks)],
            send_sem=msend_sem.at[j],
            recv_sem=mrecv_sem.at[j],
            device_id=(me - place + lax.rem(place + j, team), half),
            device_id_type=MESH,
        )

    def part_copy(g):
        at = pl.ds(pl.multiple_of(g * height, height), height)
        return pltpu.make_async_remote_copy(
            src_ref=part_out.at[at],
            dst_ref=part_in.at[at],
            send_sem=psend_sem.at[g],
            recv_sem=precv_sem.at[g],
            device_id=(me, other),
            device_id_type=MESH,
        )

    pairs = ((send_rows, rows), (send_cot, cot))
    for which, (src, dst) in enumerate(pairs):
        pass_copy(which, src.at[block(0)], 0).start()

        @pl.loop(1, count)
        def _(k):
            out_copy(which, src, dst, k).start()

    @pl.loop(1, team)
    def _(j):
        mix_copy(j).start()

    mix[pl.ds(0, toks)] = mix_in[...]
    for which, (src, dst) in enumerate(pairs):
        dst[half, pl.ds(0, cap)] = src[pl.ds(0, cap)]
    for load in loads:
        load.wait()

    def gather_group(which, g):
        src, dst = pairs[which]

        @pl.loop(0, per)
        def _(j):
            k = g * per + j

            @pl.when(k > 0)
            def _():
                out_copy(which, src, dst, k).wait_recv()
                pass_copy(which, dst.at[half, block(k)], k).start()

        @pl.loop(0, per)
        def _(j):
            k = g * per + j
            pass_copy(which, dst.at[half, block(k)], k).wait_recv()

    @pl.loop(0, GROUPS)
    def _(g):
        gather_group(0, g)
        at = pl.ds(pl.multiple_of(g * height, height), height)
        left, right = rows[0, at], rows[1, at]
        pre_g[at] = dot(left, wg[:width], 1, 0) + dot(right, wg[width:], 1, 0)
        pre_u[at] = dot(left, wu[:width], 1, 0) + dot(right, wu[width:], 1, 0)

    mine_at = pl.ds(pl.multiple_of(half * width, width), width)
    other_at = pl.ds(pl.multiple_of(other * width, width), width)

    @pl.loop(0, GROUPS)
    def _(g):
        gather_group(1, g)
        at = pl.ds(pl.multiple_of(g * height, height), height)
        grad = dot(cot[0, at], wd[:, :width], 1, 1) + dot(cot[1, at], wd[:, width:], 1, 1)
        pg, pu = pre_g[at], pre_u[at]
        sig = jax.nn.sigmoid(pg)
        silu = pg * sig
        hidden[at] = (silu * pu).astype(BF16)
        ug_now = (grad * silu).astype(BF16)
        gg_now = (grad * pu * sig * (1.0 + pg * (1.0 - sig))).astype(BF16)
        ug[at] = ug_now
        gg[at] = gg_now
        far = dot(gg_now, wg[other_at], 1, 1) + dot(ug_now, wu[other_at], 1, 1)
        part_out[at] = far.astype(BF16)
        part_copy(g).start()
        near = dot(gg_now, wg[mine_at], 1, 1) + dot(ug_now, wu[mine_at], 1, 1)
        near = near.astype(BF16).astype(F32)
        part_copy(g).wait_recv()
        ret[at] = (near + part_in[at].astype(F32)).astype(BF16)

        @pl.loop(0, per)
        def _(j):
            k = g * per + j

            @pl.when(k > 0)
            def _():
                back_copy(k).start()

    back[pl.ds(0, cap)] = ret[pl.ds(0, cap)]

    tile = 256
    per_half = width // tile

    @pl.loop(0, 2 * per_half)
    def _(t):
        h, c = t // per_half, lax.rem(t, per_half)
        cols = pl.ds(pl.multiple_of(c * tile, tile), tile)
        to = pl.ds(pl.multiple_of(t * tile, tile), tile)
        x = rows[h, :, cols].T
        gate_f[to] = dot(x, gg[...], 1, 0).astype(BF16)
        up_f[to] = dot(x, ug[...], 1, 0).astype(BF16)

    stores = [
        pltpu.make_async_copy(gate_f, gate_out.at[0], out_sem.at[0]),
        pltpu.make_async_copy(up_f, up_out.at[0], out_sem.at[1]),
    ]
    for store in stores:
        store.start()

    hid_tile = min(256, hidden.shape[1])

    @pl.loop(0, hidden.shape[1] // hid_tile)
    def _(t):
        to = pl.ds(pl.multiple_of(t * hid_tile, hid_tile), hid_tile)
        x = hidden[:, to].T
        for h in range(2):
            down_f[to, h * width : (h + 1) * width] = dot(x, cot[h], 1, 0).astype(BF16)

    stores.append(pltpu.make_async_copy(down_f, down_out.at[0], out_sem.at[2]))
    stores[-1].start()

    for which, (src, dst) in enumerate(pairs):

        @pl.loop(0, count)
        def _(k):
            @pl.when(k > 0)
            def _():
                out_copy(which, src, dst, k).wait_send()

            pass_copy(which, dst.at[half, block(k)], k).wait_send()

    @pl.loop(0, GROUPS)
    def _(g):
        part_copy(g).wait_send()

    @pl.loop(1, count)
    def _(k):
        back_copy(k).wait_send()
        back_copy(k).wait_recv()

    @pl.loop(1, team)
    def _(j):
        mix_copy(j).wait_send()
        mix_copy(j).wait_recv()

    mix_out[...] = mix[...]
    back_out[...] = back[...]
    for store in stores:
        store.wait()


def expert_pass(send_rows, send_cot, w_gate, w_up, w_down, mixer_out, cap):
    tall, width = send_rows.shape
    count = lax.axis_size("sp")
    deep, hid = w_gate.shape[1:]
    team = team_size(count)
    vmem = pl.BlockSpec(memory_space=pltpu.VMEM)
    anywhere = pl.BlockSpec(memory_space=pl.ANY)
    dma = pltpu.SemaphoreType.DMA
    return pl.pallas_call(
        functools.partial(expert_kernel, count, cap),
        out_shape=(
            jax.ShapeDtypeStruct((tall, width), BF16),
            jax.ShapeDtypeStruct((team * mixer_out.shape[0], mixer_out.shape[1]), BF16),
            jax.ShapeDtypeStruct((1, deep, hid), BF16),
            jax.ShapeDtypeStruct((1, deep, hid), BF16),
            jax.ShapeDtypeStruct((1, hid, deep), BF16),
        ),
        in_specs=[vmem, vmem, anywhere, anywhere, anywhere, vmem],
        out_specs=(vmem, vmem, anywhere, anywhere, anywhere),
        scratch_shapes=[
            pltpu.VMEM((2, tall, width), BF16),
            pltpu.VMEM((2, tall, width), BF16),
            pltpu.VMEM((deep, hid), BF16),
            pltpu.VMEM((deep, hid), BF16),
            pltpu.VMEM((hid, deep), BF16),
            pltpu.VMEM((tall, hid), F32),
            pltpu.VMEM((tall, hid), F32),
            pltpu.VMEM((tall, hid), BF16),
            pltpu.VMEM((tall, hid), BF16),
            pltpu.VMEM((tall, hid), BF16),
            pltpu.VMEM((tall, width), BF16),
            pltpu.VMEM((tall, width), BF16),
            pltpu.VMEM((tall, width), BF16),
            pltpu.VMEM((tall, width), BF16),
            pltpu.VMEM((deep, hid), BF16),
            pltpu.VMEM((deep, hid), BF16),
            pltpu.VMEM((hid, deep), BF16),
            pltpu.VMEM((team * mixer_out.shape[0], mixer_out.shape[1]), BF16),
            dma((3,)),
            dma((3,)),
            dma((2, count)),
            dma((2, count)),
            dma((2, count)),
            dma((2, count)),
            dma((GROUPS,)),
            dma((GROUPS,)),
            dma((count,)),
            dma((count,)),
            dma((team,)),
            dma((team,)),
        ],
        compiler_params=pltpu.CompilerParams(
            collective_id=0, has_side_effects=True, vmem_limit_bytes=60 * 1024 * 1024
        ),
    )(send_rows, send_cot, w_gate, w_up, w_down, mixer_out)


def mixer_kernel(
    count,
    sh,
    w_out_hbm,
    mix,
    gate_in,
    wog_out,
    mg_out,
    halo_out,
    far,
    w_out,
    sg,
    p_send,
    p_recv,
    h_send,
    h_recv,
    w_sem,
    whole_sem,
    gsend_sem,
    grecv_sem,
    fsend_sem,
    frecv_sem,
    own_sem,
    psend_sem,
    precv_sem,
    hsem,
):
    me = lax.axis_index("sp")
    half = lax.axis_index("tp")
    other = 1 - half
    team = team_size(count)
    layers = count // team
    place, layer = lax.rem(me, team), me // team
    toks, width = sh.shape
    per = layers // 2
    blk = width // (team * per)
    load = pltpu.make_async_copy(w_out_hbm, w_out, w_sem)
    load.start()

    def member(j):
        return me - place + lax.rem(place + j, team)

    def floor(i):
        return lax.rem(layer + i, layers) * team + place

    after, before = lax.rem(me + 1, count), lax.rem(me + count - 1, count)
    barrier = pltpu.get_barrier_semaphore()

    def greet(device):
        pl.semaphore_signal(barrier, inc=1, device_id=device, device_id_type=MESH)

    for j in range(1, team):
        greet((member(j), half))
    for i in range(1, layers):
        greet((floor(i), half))
    greet((me, other))
    greet((after, half))
    greet((before, half))
    pl.semaphore_wait(barrier, team - 1 + layers - 1 + 3)

    def remote(src, dst, send, recv, device):
        return pltpu.make_async_remote_copy(
            src_ref=src,
            dst_ref=dst,
            send_sem=send,
            recv_sem=recv,
            device_id=device,
            device_id_type=MESH,
        )

    def cols(j, m):
        at = (lax.rem(place + j, team) + team * m) * blk
        return pl.ds(pl.multiple_of(at, blk), blk)

    def spot(h, m, size):
        return pl.ds(pl.multiple_of((h * per + m) * blk, blk), size)

    def stripe(j):
        return pl.ds(j * toks, toks)

    def piece(j, m):
        return remote(
            sh.at[:, cols(j, m)],
            sg.at[stripe(j), spot(half, m, blk)],
            gsend_sem.at[j, m],
            grecv_sem.at[j, m],
            (member(j), half),
        )

    def own_piece(m):
        return remote(
            sh.at[:, cols(0, m)],
            sg.at[stripe(0), spot(half, m, blk)],
            own_sem.at[0, m],
            own_sem.at[1, m],
            (me, other),
        )

    def handed(j):
        ref = sg.at[stripe(j), spot(half, 0, per * blk)]
        return remote(ref, ref, fsend_sem.at[j], frecv_sem.at[j], (me, other))

    whole = remote(sh, far, whole_sem.at[0], whole_sem.at[1], (me, other))
    whole.start()
    for j in range(1, team):
        for m in range(per):
            piece(j, m).start()
    for m in range(per):
        own_piece(m).start()
        sg[stripe(0), spot(half, m, blk)] = sh[:, cols(0, m)]

    load.wait()
    near_at = pl.ds(pl.multiple_of(half * width, width), width)
    far_at = pl.ds(pl.multiple_of(other * width, width), width)
    grad = dot(sh[...], w_out[near_at], 1, 0)
    whole.wait_recv()
    grad = (grad + dot(far[...], w_out[far_at], 1, 0)).astype(BF16)
    mg_out[...] = grad
    h_send[...] = grad[:8].astype(F32) * gate_in[:8].astype(F32)
    halo = remote(h_send, h_recv, hsem.at[0], hsem.at[1], (before, half))
    halo.start()
    for j in range(1, team):
        for m in range(per):
            piece(j, m).wait_recv()
        handed(j).start()
    for m in range(per):
        own_piece(m).wait_recv()
    for j in range(1, team):
        handed(j).wait_recv()

    def share(i):
        at = pl.ds(pl.multiple_of(lax.rem(layer + i, layers) * blk, blk), blk)
        return dot(sg[:, at].T, mix[...], 1, 0)

    def part(i):
        return remote(
            p_send.at[i], p_recv.at[i], psend_sem.at[i], precv_sem.at[i], (floor(i), half)
        )

    @pl.loop(1, layers)
    def _(i):
        p_send[i] = share(i).astype(BF16)
        part(i).start()

    wog_out[...] = share(0)
    for m in range(per):
        own_piece(m).wait_send()
    whole.wait_send()
    for j in range(1, team):
        for m in range(per):
            piece(j, m).wait_send()
        handed(j).wait_send()
    halo.wait_send()
    halo.wait_recv()
    halo_out[...] = h_recv[...]

    @pl.loop(1, layers)
    def _(i):
        part(i).wait_recv()
        wog_out[...] += p_recv[i].astype(F32)

    @pl.loop(1, layers)
    def _(i):
        part(i).wait_send()


def mixer_pass(stream_half, w_out, mix, gate_in):
    count = lax.axis_size("sp")
    team = team_size(count)
    layers = count // team
    per = layers // 2
    toks, width = stream_half.shape
    deep, chans = w_out.shape
    blk = deep // count
    vmem = pl.BlockSpec(memory_space=pltpu.VMEM)
    dma = pltpu.SemaphoreType.DMA
    return pl.pallas_call(
        functools.partial(mixer_kernel, count),
        out_shape=(
            jax.ShapeDtypeStruct((blk, chans), F32),
            jax.ShapeDtypeStruct((toks, chans), BF16),
            jax.ShapeDtypeStruct((8, chans), F32),
        ),
        in_specs=[vmem, pl.BlockSpec(memory_space=pl.ANY), vmem, vmem],
        out_specs=(vmem, vmem, vmem),
        scratch_shapes=[
            pltpu.VMEM((toks, width), BF16),
            pltpu.VMEM((deep, chans), BF16),
            pltpu.VMEM((team * toks, layers * blk), BF16),
            pltpu.VMEM((layers, blk, chans), BF16),
            pltpu.VMEM((layers, blk, chans), BF16),
            pltpu.VMEM((8, chans), F32),
            pltpu.VMEM((8, chans), F32),
            dma,
            dma((2,)),
            dma((team, per)),
            dma((team, per)),
            dma((team,)),
            dma((team,)),
            dma((2, per)),
            dma((layers,)),
            dma((layers,)),
            dma((2,)),
        ],
        compiler_params=pltpu.CompilerParams(
            collective_id=1, has_side_effects=True, vmem_limit_bytes=32 * 1024 * 1024
        ),
    )(stream_half, w_out, mix, gate_in)


def shards(
    stream,
    out_grad,
    gate_in,
    conv_gate,
    conv_value,
    taps,
    w_out,
    route_ids,
    route_weights,
    w_gate,
    w_up,
    w_down,
):
    tok_rows, half_width = stream.shape
    top_count = route_ids.shape[1]
    experts = w_gate.shape[0] * lax.axis_size("sp")
    capacity = 4 * tok_rows // experts
    route_total = tok_rows * top_count
    slots = experts * capacity
    me = lax.axis_index("sp")
    relative = lax.rem(route_ids - me + experts, experts)
    flat = relative.reshape(route_total)
    one_hot = flat[:, None] == jnp.arange(experts, dtype=jnp.int32)[None, :]
    order = jnp.arange(route_total, dtype=jnp.int32)
    earlier = (order[:, None] > order[None, :]).astype(BF16)
    ranks = dot(earlier, one_hot.astype(BF16), 1, 0)
    slot_pos = jnp.sum(jnp.where(one_hot, ranks, 0.0), axis=1).astype(jnp.int32)
    slot_of = (flat * capacity + slot_pos).reshape(tok_rows, top_count)
    places = jnp.arange(slots, dtype=jnp.int32)
    hits = [slot_of[:, k][None, :] == places[:, None] for k in range(top_count)]
    slot_weight = sum(
        jnp.sum(jnp.where(hits[k], route_weights[:, k][None, :], 0.0), axis=1)
        for k in range(top_count)
    )
    pick = functools.reduce(jnp.logical_or, hits).astype(BF16)
    send_rows = dot(pick, stream, 1, 0).astype(BF16)
    send_cot = (slot_weight[:, None] * dot(pick, out_grad, 1, 0)).astype(BF16)
    depth = taps.shape[0]
    channels = conv_gate.shape[1]
    prod_rows = conv_gate.astype(jnp.float32) * conv_value.astype(jnp.float32)
    left_rows = passed_along(prod_rows[tok_rows - depth + 1 :], "sp", 1)
    padded = jnp.concatenate([left_rows, prod_rows], axis=0)
    conv_sum = jnp.zeros((tok_rows, channels), jnp.float32)
    for tap_index in range(depth):
        conv_sum = conv_sum + taps[tap_index][None, :] * padded[tap_index : tap_index + tok_rows]
    mixer_out = (gate_in.astype(jnp.float32) * conv_sum).astype(jnp.bfloat16)
    back, mix, gate_w_grad, up_w_grad, down_w_grad = expert_pass(
        send_rows, send_cot, w_gate, w_up, w_down, mixer_out, capacity
    )
    input_grad = dot(pick, back, 0, 0)
    stream_half = (out_grad.astype(jnp.float32) + input_grad).astype(jnp.bfloat16)
    if w_out.shape[0] // lax.axis_size("sp") % 128 == 0:
        out_proj_grad, mixer_grad, halo = mixer_pass(stream_half, w_out, mix, gate_in)
    else:
        stream_whole = lax.all_gather(stream_half, "tp", axis=1, tiled=True)
        mixer_grad = dot(stream_whole, w_out, 1, 0).astype(BF16)
        out_proj_grad = lax.psum_scatter(
            dot(stream_whole, mixer_out, 0, 0).astype(BF16), "sp", scatter_dimension=0, tiled=True
        ).astype(F32)
        first = mixer_grad[: depth - 1].astype(F32) * gate_in[: depth - 1].astype(F32)
        halo = passed_along(first, "sp", -1)
    mixer_wide = mixer_grad.astype(jnp.float32)
    gate_in_grad = (mixer_wide * conv_sum).astype(jnp.bfloat16)
    conv_inner = mixer_wide * gate_in.astype(jnp.float32)
    right_rows = jnp.where(me == lax.axis_size("sp") - 1, 0.0, halo[: depth - 1])
    padded_back = jnp.concatenate([conv_inner, right_rows], axis=0)
    prod_grad = jnp.zeros((tok_rows, channels), jnp.float32)
    for tap_index in range(depth):
        offset = depth - 1 - tap_index
        prod_grad = prod_grad + taps[tap_index][None, :] * padded_back[offset : offset + tok_rows]
    conv_gate_grad = (prod_grad * conv_value.astype(jnp.float32)).astype(jnp.bfloat16)
    conv_value_grad = (prod_grad * conv_gate.astype(jnp.float32)).astype(jnp.bfloat16)
    return (
        stream_half,
        gate_in_grad,
        conv_gate_grad,
        conv_value_grad,
        out_proj_grad,
        gate_w_grad.astype(F32),
        up_w_grad.astype(F32),
        down_w_grad.astype(F32),
    )


def solution(mesh):
    placed = (
        P("sp", "tp"),
        P("sp", "tp"),
        P("sp", "tp"),
        P("sp", "tp"),
        P("sp", "tp"),
        P(None, "tp"),
        P(None, "tp"),
        P("sp", None),
        P("sp", None),
        P("sp", None, "tp"),
        P("sp", None, "tp"),
        P("sp", "tp", None),
    )
    return jax.shard_map(
        shards,
        mesh=mesh,
        in_specs=placed,
        out_specs=(
            P("sp", "tp"),
            P("sp", "tp"),
            P("sp", "tp"),
            P("sp", "tp"),
            P("sp", "tp"),
            P("sp", None, "tp"),
            P("sp", None, "tp"),
            P("sp", "tp", None),
        ),
        check_vma=False,
    )
```

```python
import functools

import jax
import jax.numpy as jnp
from jax import lax
from jax.experimental import pallas as pl
from jax.experimental.pallas import tpu as pltpu
from jax.sharding import PartitionSpec as P

MESH = pl.DeviceIdType.MESH
GROUPS = 4
F32 = jnp.float32
BF16 = jnp.bfloat16


def passed_along(shard, axis, by):
    count = lax.axis_size(axis)
    pairs = [(i, i + by) for i in range(count) if 0 <= i + by < count]
    return lax.ppermute(shard, axis, pairs)


def dot(a, b, ca, cb):
    return lax.dot_general(a, b, (((ca,), (cb,)), ((), ())), preferred_element_type=F32)


def team_size(count):
    size = 1
    while size * size < count:
        size *= 2
    return size


def expert_kernel(
    count,
    cap,
    send_rows,
    send_cot,
    wg_hbm,
    wu_hbm,
    wd_hbm,
    mix_in,
    stream_in,
    grad_in,
    pick,
    scale,
    back_out,
    cross_out,
    mix_out,
    gate_out,
    up_out,
    down_out,
    rows,
    cot,
    wg,
    wu,
    wd,
    pre_g,
    pre_u,
    hidden,
    gg,
    ug,
    part_out,
    part_in,
    ret,
    back,
    gate_f,
    up_f,
    down_f,
    mix,
    toks_in,
    rel_rows,
    rel_cot,
    cross_src,
    cross_dst,
    x_send,
    x_recv,
    w_sem,
    out_sem,
    send_sem,
    recv_sem,
    fsend_sem,
    frecv_sem,
    psend_sem,
    precv_sem,
    rsend_sem,
    rrecv_sem,
    msend_sem,
    mrecv_sem,
):
    me = lax.axis_index("sp")
    half = lax.axis_index("tp")
    other = 1 - half
    per = count // GROUPS
    height = per * cap
    width = rows.shape[2]
    ring = count // 2
    loc = lax.rem(me, ring)
    base = me - loc
    mirror = (lax.rem(me + ring, count), half)

    loads = []
    for n, (a, b) in enumerate(((wg_hbm, wg), (wu_hbm, wu), (wd_hbm, wd))):
        load = pltpu.make_async_copy(a.at[0], b, w_sem.at[n])
        load.start()
        loads.append(load)

    barrier = pltpu.get_barrier_semaphore()

    @pl.loop(1, ring)
    def _(k):
        pl.semaphore_signal(
            barrier, inc=1, device_id=(base + lax.rem(loc + k, ring), half), device_id_type=MESH
        )

    pl.semaphore_signal(barrier, inc=1, device_id=(me, other), device_id_type=MESH)
    pl.semaphore_signal(barrier, inc=1, device_id=mirror, device_id_type=MESH)
    pl.semaphore_wait(barrier, ring + 1)

    def block(k):
        return pl.ds(pl.multiple_of(k * cap, cap), cap)

    def out_copy(which, src, dst, k):
        return pltpu.make_async_remote_copy(
            src_ref=src.at[block(lax.rem(k, ring))],
            dst_ref=dst.at[half, block(k)],
            send_sem=send_sem.at[which, k],
            recv_sem=recv_sem.at[which, k],
            device_id=(base + lax.rem(loc + k, ring), half),
            device_id_type=MESH,
        )

    def pass_copy(which, src, k):
        return pltpu.make_async_remote_copy(
            src_ref=src,
            dst_ref=(rows if which == 0 else cot).at[half, block(k)],
            send_sem=fsend_sem.at[which, k],
            recv_sem=frecv_sem.at[which, k],
            device_id=(me, other),
            device_id_type=MESH,
        )

    def back_copy(k):
        return pltpu.make_async_remote_copy(
            src_ref=ret.at[block(k)],
            dst_ref=back.at[block(k)],
            send_sem=rsend_sem.at[k],
            recv_sem=rrecv_sem.at[k],
            device_id=(base + lax.rem(loc - k + 2 * ring, ring), half),
            device_id_type=MESH,
        )

    team = team_size(count)
    place = lax.rem(me, team)
    toks = mix_in.shape[0]

    def mix_copy(j):
        return pltpu.make_async_remote_copy(
            src_ref=mix_in,
            dst_ref=mix.at[pl.ds(pl.multiple_of(j * toks, toks), toks)],
            send_sem=msend_sem.at[j],
            recv_sem=mrecv_sem.at[j],
            device_id=(me - place + lax.rem(place + j, team), half),
            device_id_type=MESH,
        )

    def part_copy(g):
        at = pl.ds(pl.multiple_of(g * height, height), height)
        return pltpu.make_async_remote_copy(
            src_ref=part_out.at[at],
            dst_ref=part_in.at[at],
            send_sem=psend_sem.at[g],
            recv_sem=precv_sem.at[g],
            device_id=(me, other),
            device_id_type=MESH,
        )

    def cross_copy(n, src, dst):
        return pltpu.make_async_remote_copy(
            src_ref=src,
            dst_ref=dst,
            send_sem=x_send.at[n],
            recv_sem=x_recv.at[n],
            device_id=mirror,
            device_id_type=MESH,
        )

    crossing = (
        cross_copy(0, stream_in, toks_in.at[0]),
        cross_copy(1, grad_in, toks_in.at[1]),
        cross_copy(2, cross_src, cross_dst),
    )
    crossing[0].start()
    crossing[1].start()
    pairs = ((send_rows, rows), (send_cot, cot))
    for which, (src, dst) in enumerate(pairs):
        pass_copy(which, src.at[block(0)], 0).start()

        @pl.loop(1, ring)
        def _(k):
            out_copy(which, src, dst, k).start()

    @pl.loop(1, team)
    def _(j):
        mix_copy(j).start()

    mix[pl.ds(0, toks)] = mix_in[...]
    for which, (src, dst) in enumerate(pairs):
        dst[half, pl.ds(0, cap)] = src[pl.ds(0, cap)]
    for which, (rel, dst) in enumerate(((rel_rows, rows), (rel_cot, cot))):
        crossing[which].wait_recv()
        chosen = dot(pick[...], toks_in[which], 1, 0)
        chosen = (chosen if which == 0 else scale[...] * chosen).astype(BF16)
        rel[...] = chosen
        dst[half, pl.ds(ring * cap, cap)] = chosen[:cap]
        pass_copy(which, rel.at[block(0)], ring).start()

        @pl.loop(ring + 1, count)
        def _(k):
            out_copy(which, rel, dst, k).start()

    for load in loads:
        load.wait()

    def gather_group(which, g):
        src, dst = pairs[which]

        @pl.loop(0, per)
        def _(j):
            k = g * per + j

            @pl.when(lax.rem(k, ring) > 0)
            def _():
                out_copy(which, src, dst, k).wait_recv()
                pass_copy(which, dst.at[half, block(k)], k).start()

        @pl.loop(0, per)
        def _(j):
            k = g * per + j
            pass_copy(which, dst.at[half, block(k)], k).wait_recv()

    @pl.loop(0, GROUPS)
    def _(g):
        gather_group(0, g)
        at = pl.ds(pl.multiple_of(g * height, height), height)
        left, right = rows[0, at], rows[1, at]
        pre_g[at] = dot(left, wg[:width], 1, 0) + dot(right, wg[width:], 1, 0)
        pre_u[at] = dot(left, wu[:width], 1, 0) + dot(right, wu[width:], 1, 0)

    mine_at = pl.ds(pl.multiple_of(half * width, width), width)
    other_at = pl.ds(pl.multiple_of(other * width, width), width)

    @pl.loop(0, GROUPS)
    def _(g):
        gather_group(1, g)
        at = pl.ds(pl.multiple_of(g * height, height), height)
        grad = dot(cot[0, at], wd[:, :width], 1, 1) + dot(cot[1, at], wd[:, width:], 1, 1)
        pg, pu = pre_g[at], pre_u[at]
        sig = jax.nn.sigmoid(pg)
        silu = pg * sig
        hidden[at] = (silu * pu).astype(BF16)
        ug_now = (grad * silu).astype(BF16)
        gg_now = (grad * pu * sig * (1.0 + pg * (1.0 - sig))).astype(BF16)
        ug[at] = ug_now
        gg[at] = gg_now
        far = dot(gg_now, wg[other_at], 1, 1) + dot(ug_now, wu[other_at], 1, 1)
        part_out[at] = far.astype(BF16)
        part_copy(g).start()
        near = dot(gg_now, wg[mine_at], 1, 1) + dot(ug_now, wu[mine_at], 1, 1)
        near = near.astype(BF16).astype(F32)
        part_copy(g).wait_recv()
        ret[at] = (near + part_in[at].astype(F32)).astype(BF16)

        @pl.loop(0, per)
        def _(j):
            k = g * per + j

            @pl.when(lax.rem(k, ring) > 0)
            def _():
                back_copy(k).start()

    back[pl.ds(0, cap)] = ret[pl.ds(0, cap)]
    back[pl.ds(ring * cap, cap)] = ret[pl.ds(ring * cap, cap)]

    tile = 256
    per_half = width // tile

    @pl.loop(0, 2 * per_half)
    def _(t):
        h, c = t // per_half, lax.rem(t, per_half)
        cols = pl.ds(pl.multiple_of(c * tile, tile), tile)
        to = pl.ds(pl.multiple_of(t * tile, tile), tile)
        x = rows[h, :, cols].T
        gate_f[to] = dot(x, gg[...], 1, 0).astype(BF16)
        up_f[to] = dot(x, ug[...], 1, 0).astype(BF16)

    stores = [
        pltpu.make_async_copy(gate_f, gate_out.at[0], out_sem.at[0]),
        pltpu.make_async_copy(up_f, up_out.at[0], out_sem.at[1]),
    ]
    for store in stores:
        store.start()

    hid_tile = min(256, hidden.shape[1])

    @pl.loop(0, hidden.shape[1] // hid_tile)
    def _(t):
        to = pl.ds(pl.multiple_of(t * hid_tile, hid_tile), hid_tile)
        x = hidden[:, to].T
        for h in range(2):
            down_f[to, h * width : (h + 1) * width] = dot(x, cot[h], 1, 0).astype(BF16)

    stores.append(pltpu.make_async_copy(down_f, down_out.at[0], out_sem.at[2]))
    stores[-1].start()

    @pl.loop(ring + 1, count)
    def _(k):
        back_copy(k).wait_recv()

    cross_src[...] = dot(pick[...], back[ring * cap :], 0, 0).astype(BF16)
    crossing[2].start()

    for which, (src, dst) in enumerate(pairs):

        @pl.loop(0, count)
        def _(k):
            @pl.when(lax.rem(k, ring) > 0)
            def _():
                out_copy(which, src, dst, k).wait_send()

            pass_copy(which, dst.at[half, block(k)], k).wait_send()

    @pl.loop(0, GROUPS)
    def _(g):
        part_copy(g).wait_send()

    @pl.loop(1, ring)
    def _(k):
        back_copy(k).wait_send()
        back_copy(k).wait_recv()

    @pl.loop(ring + 1, count)
    def _(k):
        back_copy(k).wait_send()

    @pl.loop(1, team)
    def _(j):
        mix_copy(j).wait_send()
        mix_copy(j).wait_recv()

    mix_out[...] = mix[...]
    back_out[...] = back[: ring * cap]
    for copy in crossing:
        copy.wait_send()
    crossing[2].wait_recv()
    cross_out[...] = cross_dst[...]
    for store in stores:
        store.wait()


def expert_pass(
    send_rows, send_cot, w_gate, w_up, w_down, mixer_out, stream, out_grad, pick, scale, cap
):
    short, width = send_rows.shape
    tall = 2 * short
    toks = stream.shape[0]
    count = lax.axis_size("sp")
    deep, hid = w_gate.shape[1:]
    team = team_size(count)
    vmem = pl.BlockSpec(memory_space=pltpu.VMEM)
    anywhere = pl.BlockSpec(memory_space=pl.ANY)
    dma = pltpu.SemaphoreType.DMA
    return pl.pallas_call(
        functools.partial(expert_kernel, count, cap),
        out_shape=(
            jax.ShapeDtypeStruct((short, width), BF16),
            jax.ShapeDtypeStruct((toks, width), BF16),
            jax.ShapeDtypeStruct((team * mixer_out.shape[0], mixer_out.shape[1]), BF16),
            jax.ShapeDtypeStruct((1, deep, hid), BF16),
            jax.ShapeDtypeStruct((1, deep, hid), BF16),
            jax.ShapeDtypeStruct((1, hid, deep), BF16),
        ),
        in_specs=[vmem, vmem, anywhere, anywhere, anywhere] + [vmem] * 5,
        out_specs=(vmem, vmem, vmem, anywhere, anywhere, anywhere),
        scratch_shapes=[
            pltpu.VMEM((2, tall, width), BF16),
            pltpu.VMEM((2, tall, width), BF16),
            pltpu.VMEM((deep, hid), BF16),
            pltpu.VMEM((deep, hid), BF16),
            pltpu.VMEM((hid, deep), BF16),
            pltpu.VMEM((tall, hid), F32),
            pltpu.VMEM((tall, hid), F32),
            pltpu.VMEM((tall, hid), BF16),
            pltpu.VMEM((tall, hid), BF16),
            pltpu.VMEM((tall, hid), BF16),
            pltpu.VMEM((tall, width), BF16),
            pltpu.VMEM((tall, width), BF16),
            pltpu.VMEM((tall, width), BF16),
            pltpu.VMEM((tall, width), BF16),
            pltpu.VMEM((deep, hid), BF16),
            pltpu.VMEM((deep, hid), BF16),
            pltpu.VMEM((hid, deep), BF16),
            pltpu.VMEM((team * mixer_out.shape[0], mixer_out.shape[1]), BF16),
            pltpu.VMEM((2, toks, width), BF16),
            pltpu.VMEM((short, width), BF16),
            pltpu.VMEM((short, width), BF16),
            pltpu.VMEM((toks, width), BF16),
            pltpu.VMEM((toks, width), BF16),
            dma((3,)),
            dma((3,)),
            dma((3,)),
            dma((3,)),
            dma((2, count)),
            dma((2, count)),
            dma((2, count)),
            dma((2, count)),
            dma((GROUPS,)),
            dma((GROUPS,)),
            dma((count,)),
            dma((count,)),
            dma((team,)),
            dma((team,)),
        ],
        compiler_params=pltpu.CompilerParams(
            collective_id=0, has_side_effects=True, vmem_limit_bytes=60 * 1024 * 1024
        ),
    )(send_rows, send_cot, w_gate, w_up, w_down, mixer_out, stream, out_grad, pick, scale)


def mixer_kernel(
    count,
    sh,
    w_out_hbm,
    mix,
    gate_in,
    wog_out,
    mg_out,
    halo_out,
    far,
    w_out,
    sg,
    p_send,
    p_recv,
    h_send,
    h_recv,
    w_sem,
    whole_sem,
    gsend_sem,
    grecv_sem,
    fsend_sem,
    frecv_sem,
    own_sem,
    psend_sem,
    precv_sem,
    hsem,
):
    me = lax.axis_index("sp")
    half = lax.axis_index("tp")
    other = 1 - half
    team = team_size(count)
    layers = count // team
    place, layer = lax.rem(me, team), me // team
    toks, width = sh.shape
    per = layers // 2
    blk = width // (team * per)
    load = pltpu.make_async_copy(w_out_hbm, w_out, w_sem)
    load.start()

    def member(j):
        return me - place + lax.rem(place + j, team)

    def floor(i):
        return lax.rem(layer + i, layers) * team + place

    after, before = lax.rem(me + 1, count), lax.rem(me + count - 1, count)
    barrier = pltpu.get_barrier_semaphore()

    def greet(device):
        pl.semaphore_signal(barrier, inc=1, device_id=device, device_id_type=MESH)

    for j in range(1, team):
        greet((member(j), half))
    for i in range(1, layers):
        greet((floor(i), half))
    greet((me, other))
    greet((after, half))
    greet((before, half))
    pl.semaphore_wait(barrier, team - 1 + layers - 1 + 3)

    def remote(src, dst, send, recv, device):
        return pltpu.make_async_remote_copy(
            src_ref=src,
            dst_ref=dst,
            send_sem=send,
            recv_sem=recv,
            device_id=device,
            device_id_type=MESH,
        )

    def cols(j, m):
        at = (lax.rem(place + j, team) + team * m) * blk
        return pl.ds(pl.multiple_of(at, blk), blk)

    def spot(h, m, size):
        return pl.ds(pl.multiple_of((h * per + m) * blk, blk), size)

    def stripe(j):
        return pl.ds(j * toks, toks)

    def piece(j, m):
        return remote(
            sh.at[:, cols(j, m)],
            sg.at[stripe(j), spot(half, m, blk)],
            gsend_sem.at[j, m],
            grecv_sem.at[j, m],
            (member(j), half),
        )

    def own_piece(m):
        return remote(
            sh.at[:, cols(0, m)],
            sg.at[stripe(0), spot(half, m, blk)],
            own_sem.at[0, m],
            own_sem.at[1, m],
            (me, other),
        )

    def handed(j):
        ref = sg.at[stripe(j), spot(half, 0, per * blk)]
        return remote(ref, ref, fsend_sem.at[j], frecv_sem.at[j], (me, other))

    whole = remote(sh, far, whole_sem.at[0], whole_sem.at[1], (me, other))
    whole.start()
    for j in range(1, team):
        for m in range(per):
            piece(j, m).start()
    for m in range(per):
        own_piece(m).start()
        sg[stripe(0), spot(half, m, blk)] = sh[:, cols(0, m)]

    load.wait()
    near_at = pl.ds(pl.multiple_of(half * width, width), width)
    far_at = pl.ds(pl.multiple_of(other * width, width), width)
    grad = dot(sh[...], w_out[near_at], 1, 0)
    whole.wait_recv()
    grad = (grad + dot(far[...], w_out[far_at], 1, 0)).astype(BF16)
    mg_out[...] = grad
    h_send[...] = grad[:8].astype(F32) * gate_in[:8].astype(F32)
    halo = remote(h_send, h_recv, hsem.at[0], hsem.at[1], (before, half))
    halo.start()
    for j in range(1, team):
        for m in range(per):
            piece(j, m).wait_recv()
        handed(j).start()
    for m in range(per):
        own_piece(m).wait_recv()
    for j in range(1, team):
        handed(j).wait_recv()

    def share(i):
        at = pl.ds(pl.multiple_of(lax.rem(layer + i, layers) * blk, blk), blk)
        return dot(sg[:, at].T, mix[...], 1, 0)

    def part(i):
        return remote(
            p_send.at[i], p_recv.at[i], psend_sem.at[i], precv_sem.at[i], (floor(i), half)
        )

    @pl.loop(1, layers)
    def _(i):
        p_send[i] = share(i).astype(BF16)
        part(i).start()

    wog_out[...] = share(0)
    for m in range(per):
        own_piece(m).wait_send()
    whole.wait_send()
    for j in range(1, team):
        for m in range(per):
            piece(j, m).wait_send()
        handed(j).wait_send()
    halo.wait_send()
    halo.wait_recv()
    halo_out[...] = h_recv[...]

    @pl.loop(1, layers)
    def _(i):
        part(i).wait_recv()
        wog_out[...] += p_recv[i].astype(F32)

    @pl.loop(1, layers)
    def _(i):
        part(i).wait_send()


def mixer_pass(stream_half, w_out, mix, gate_in):
    count = lax.axis_size("sp")
    team = team_size(count)
    layers = count // team
    per = layers // 2
    toks, width = stream_half.shape
    deep, chans = w_out.shape
    blk = deep // count
    vmem = pl.BlockSpec(memory_space=pltpu.VMEM)
    dma = pltpu.SemaphoreType.DMA
    return pl.pallas_call(
        functools.partial(mixer_kernel, count),
        out_shape=(
            jax.ShapeDtypeStruct((blk, chans), F32),
            jax.ShapeDtypeStruct((toks, chans), BF16),
            jax.ShapeDtypeStruct((8, chans), F32),
        ),
        in_specs=[vmem, pl.BlockSpec(memory_space=pl.ANY), vmem, vmem],
        out_specs=(vmem, vmem, vmem),
        scratch_shapes=[
            pltpu.VMEM((toks, width), BF16),
            pltpu.VMEM((deep, chans), BF16),
            pltpu.VMEM((team * toks, layers * blk), BF16),
            pltpu.VMEM((layers, blk, chans), BF16),
            pltpu.VMEM((layers, blk, chans), BF16),
            pltpu.VMEM((8, chans), F32),
            pltpu.VMEM((8, chans), F32),
            dma,
            dma((2,)),
            dma((team, per)),
            dma((team, per)),
            dma((team,)),
            dma((team,)),
            dma((2, per)),
            dma((layers,)),
            dma((layers,)),
            dma((2,)),
        ],
        compiler_params=pltpu.CompilerParams(
            collective_id=1, has_side_effects=True, vmem_limit_bytes=32 * 1024 * 1024
        ),
    )(stream_half, w_out, mix, gate_in)


def shards(
    stream,
    out_grad,
    gate_in,
    conv_gate,
    conv_value,
    taps,
    w_out,
    route_ids,
    route_weights,
    w_gate,
    w_up,
    w_down,
):
    tok_rows, half_width = stream.shape
    top_count = route_ids.shape[1]
    experts = w_gate.shape[0] * lax.axis_size("sp")
    capacity = 4 * tok_rows // experts
    route_total = tok_rows * top_count
    slots = experts * capacity
    me = lax.axis_index("sp")
    ring = experts // 2
    away = (route_ids // ring != me // ring).astype(jnp.int32)
    flat = (away * ring + lax.rem(route_ids - me + experts, ring)).reshape(route_total)
    one_hot = flat[:, None] == jnp.arange(experts, dtype=jnp.int32)[None, :]
    order = jnp.arange(route_total, dtype=jnp.int32)
    earlier = (order[:, None] > order[None, :]).astype(BF16)
    ranks = dot(earlier, one_hot.astype(BF16), 1, 0)
    slot_pos = jnp.sum(jnp.where(one_hot, ranks, 0.0), axis=1).astype(jnp.int32)
    slot_of = (flat * capacity + slot_pos).reshape(tok_rows, top_count)
    short = slots // 2
    places = jnp.arange(short, dtype=jnp.int32)

    def placed_by(slot_rows, weight_rows):
        hits = [row[None, :] == places[:, None] for row in slot_rows]
        weights = sum(
            jnp.sum(jnp.where(hit, row[None, :], 0.0), axis=1)
            for hit, row in zip(hits, weight_rows)
        )
        return functools.reduce(jnp.logical_or, hits).astype(BF16), weights[:, None]

    table = jnp.concatenate([(slot_of - short).T.astype(F32), route_weights.T], axis=0)
    across = lax.ppermute(table, "sp", [(i, (i + ring) % experts) for i in range(experts)])
    pick_far, scale_far = placed_by(
        across[:top_count].astype(jnp.int32), across[top_count:]
    )
    pick, slot_weight = placed_by(slot_of.T, route_weights.T)
    send_rows = dot(pick, stream, 1, 0).astype(BF16)
    send_cot = (slot_weight * dot(pick, out_grad, 1, 0)).astype(BF16)
    depth = taps.shape[0]
    channels = conv_gate.shape[1]
    prod_rows = conv_gate.astype(jnp.float32) * conv_value.astype(jnp.float32)
    left_rows = passed_along(prod_rows[tok_rows - depth + 1 :], "sp", 1)
    padded = jnp.concatenate([left_rows, prod_rows], axis=0)
    conv_sum = jnp.zeros((tok_rows, channels), jnp.float32)
    for tap_index in range(depth):
        conv_sum = conv_sum + taps[tap_index][None, :] * padded[tap_index : tap_index + tok_rows]
    mixer_out = (gate_in.astype(jnp.float32) * conv_sum).astype(jnp.bfloat16)
    back, crossed, mix, gate_w_grad, up_w_grad, down_w_grad = expert_pass(
        send_rows,
        send_cot,
        w_gate,
        w_up,
        w_down,
        mixer_out,
        stream,
        out_grad,
        pick_far,
        scale_far,
        capacity,
    )
    input_grad = dot(pick, back, 0, 0) + crossed.astype(F32)
    stream_half = (out_grad.astype(jnp.float32) + input_grad).astype(jnp.bfloat16)
    if w_out.shape[0] // lax.axis_size("sp") % 128 == 0:
        out_proj_grad, mixer_grad, halo = mixer_pass(stream_half, w_out, mix, gate_in)
    else:
        stream_whole = lax.all_gather(stream_half, "tp", axis=1, tiled=True)
        mixer_grad = dot(stream_whole, w_out, 1, 0).astype(BF16)
        out_proj_grad = lax.psum_scatter(
            dot(stream_whole, mixer_out, 0, 0).astype(BF16), "sp", scatter_dimension=0, tiled=True
        ).astype(F32)
        first = mixer_grad[: depth - 1].astype(F32) * gate_in[: depth - 1].astype(F32)
        halo = passed_along(first, "sp", -1)
    mixer_wide = mixer_grad.astype(jnp.float32)
    gate_in_grad = (mixer_wide * conv_sum).astype(jnp.bfloat16)
    conv_inner = mixer_wide * gate_in.astype(jnp.float32)
    right_rows = jnp.where(me == lax.axis_size("sp") - 1, 0.0, halo[: depth - 1])
    padded_back = jnp.concatenate([conv_inner, right_rows], axis=0)
    prod_grad = jnp.zeros((tok_rows, channels), jnp.float32)
    for tap_index in range(depth):
        offset = depth - 1 - tap_index
        prod_grad = prod_grad + taps[tap_index][None, :] * padded_back[offset : offset + tok_rows]
    conv_gate_grad = (prod_grad * conv_value.astype(jnp.float32)).astype(jnp.bfloat16)
    conv_value_grad = (prod_grad * conv_gate.astype(jnp.float32)).astype(jnp.bfloat16)
    return (
        stream_half,
        gate_in_grad,
        conv_gate_grad,
        conv_value_grad,
        out_proj_grad,
        gate_w_grad.astype(F32),
        up_w_grad.astype(F32),
        down_w_grad.astype(F32),
    )


def solution(mesh):
    placed = (
        P("sp", "tp"),
        P("sp", "tp"),
        P("sp", "tp"),
        P("sp", "tp"),
        P("sp", "tp"),
        P(None, "tp"),
        P(None, "tp"),
        P("sp", None),
        P("sp", None),
        P("sp", None, "tp"),
        P("sp", None, "tp"),
        P("sp", "tp", None),
    )
    return jax.shard_map(
        shards,
        mesh=mesh,
        in_specs=placed,
        out_specs=(
            P("sp", "tp"),
            P("sp", "tp"),
            P("sp", "tp"),
            P("sp", "tp"),
            P("sp", "tp"),
            P("sp", None, "tp"),
            P("sp", None, "tp"),
            P("sp", "tp", None),
        ),
        check_vma=False,
    )
```
